32 devices in a mesh: rep: 2 (over x), fs: 4 (over z), tp: 4 (over y, core).
Axes of the slice: x: 2, y: 2, z: 4, core: 2. Of those that a mesh axis runs over, the one named last changes fastest.
Arguments:
- tokens: bfloat16 [8192, 2048], P(('rep', 'fs'), 'tp'), may hold values from -6 to 6
- mix_gain: float32 [2048], replicated, may hold values from 0.1 to 1.9
- query_weight: bfloat16 [2048, 512], P('fs', 'tp'), may hold values from -0.125 to 0.125
- key_weight: bfloat16 [2048, 512], P('fs', 'tp'), may hold values from -0.125 to 0.125
- value_weight: bfloat16 [2048, 1024], P('fs', 'tp'), may hold values from -0.125 to 0.125
- gate_weight: bfloat16 [2048, 1024], P('fs', 'tp'), may hold values from -0.125 to 0.125
- out_weight: bfloat16 [1024, 2048], P('tp', 'fs'), may hold values from -0.1875 to 0.1875
- head_gain: float32 [8, 128], P('tp'), may hold values from 0.1 to 1.9
- ffn_gain: float32 [2048], replicated, may hold values from 0.1 to 1.9
- ffn_gate: bfloat16 [2048, 5632], P('fs', 'tp'), may hold values from -0.125 to 0.125
- ffn_up: bfloat16 [2048, 5632], P('fs', 'tp'), may hold values from -0.125 to 0.125
- ffn_down: bfloat16 [5632, 2048], P('tp', 'fs'), may hold values from -0.078125 to 0.078125
Outputs:
- layer_out: bfloat16 [8192, 2048], P(('rep', 'fs'), 'tp')
The draws below stay inside these ranges and needn't reach their ends.
All inputs are finite; a program needn't handle non-finite values.
Results may differ from the reference program's by a relative error of at most 0.03.
Values may be sent and summed in bfloat16 or wider, within the bound.
A program may use at most 128 MiB of HBM per device.

```python
import jax
import jax.numpy as jnp
from jax import lax

D = 2048
HEADS = 8
DK = 64
DV = 128
FF = 5632
SEQ = 256
TOKENS = 8192
N_TP = 4


def levels(rng, extent, shards, least, largest):
    gain = 1.0
    for dim, parts in shards:
        steps = jax.random.uniform(jax.random.fold_in(jax.random.fold_in(rng, 6), dim), (parts,), jnp.float32, least / len(shards), largest / len(shards))
        gain = gain * jnp.repeat(jnp.exp(steps), extent[dim] // parts).reshape((-1,) + (1,) * (len(extent) - 1 - dim))
    return gain


def normal_values(key, extent, scale, most, shards=(), held_as=jnp.bfloat16):
    level = levels(key, extent, shards, -0.22, 0.18) if shards else 1.0
    values = jax.random.normal(key, extent, jnp.float32) * scale * level
    return jnp.minimum(jnp.maximum(values, -most), most).astype(held_as)


def setup_inputs(seed: int = 0) -> dict:
    seeds = jax.random.split(jax.random.key(seed), 13)
    return {
        "tokens": normal_values(seeds[0], (TOKENS, D), 1.0, 6.0, ((0, 8), (1, 4))),
        "mix_gain": jnp.clip(1.0 + 0.18 * jax.random.normal(seeds[1], (D,), jnp.float32), 0.1, 1.9),
        "query_weight": normal_values(seeds[2], (D, HEADS * DK), D ** -0.5, 0.125, ((0, 4), (1, 4))),
        "key_weight": normal_values(seeds[3], (D, HEADS * DK), D ** -0.5, 0.125, ((0, 4), (1, 4))),
        "value_weight": normal_values(seeds[4], (D, HEADS * DV), D ** -0.5, 0.125, ((0, 4), (1, 4))),
        "gate_weight": normal_values(seeds[5], (D, HEADS * DV), D ** -0.5, 0.125, ((0, 4), (1, 4))),
        "out_weight": normal_values(seeds[6], (HEADS * DV, D), (HEADS * DV) ** -0.5, 0.1875, ((0, 4), (1, 4))),
        "head_gain": jnp.clip(1.0 + 0.18 * jax.random.normal(seeds[7], (HEADS, DV), jnp.float32), 0.1, 1.9),
        "ffn_gain": jnp.clip(1.0 + 0.18 * jax.random.normal(seeds[8], (D,), jnp.float32), 0.1, 1.9),
        "ffn_gate": normal_values(seeds[9], (D, FF), D ** -0.5, 0.125, ((0, 4), (1, 4))),
        "ffn_up": normal_values(seeds[10], (D, FF), D ** -0.5, 0.125, ((0, 4), (1, 4))),
        "ffn_down": normal_values(seeds[11], (FF, D), FF ** -0.5, 0.078125, ((0, 4), (1, 4))),
    }


epsilon = 1e-06
rope_base = 10000.0

def norm_rows(values, gain_row):
    floats = values.astype(jnp.float32)
    scaled = floats * lax.rsqrt(lax.optimization_barrier(jnp.mean(floats * floats, axis=-1, keepdims=True)) + epsilon)
    return (scaled * gain_row).astype(jnp.bfloat16)

def rotate(values, positions):
    half_dim = values.shape[-1] // 2
    frequency = rope_base ** (-jnp.linspace(0.0, 1.0, half_dim, dtype=jnp.float32))
    angles = positions.astype(jnp.float32)[:, None] * frequency[None, :]
    cosine = jnp.cos(angles)[:, None, :]
    sine_part = jnp.sin(angles)[:, None, :]
    paired = values.reshape(values.shape[:-1] + (half_dim, 2))
    leading = paired[..., 0]
    trailing = paired[..., 1]
    turned = jnp.stack([leading * cosine - trailing * sine_part, leading * sine_part + trailing * cosine], axis=-1)
    return turned.reshape(values.shape)

def log_decay(head_index, total_heads):
    return jnp.log1p(-jnp.exp2(-5.0 - 4.0 * head_index.astype(jnp.float32) / (total_heads - 1)))

def split_sum(left, right):
    columns = left.shape[1] // N_TP
    summed = jnp.zeros((left.shape[0], right.shape[1]), jnp.float32)
    for segment in range(N_TP):
        partial_value = jnp.dot(left[:, segment * columns:(segment + 1) * columns], right[segment * columns:(segment + 1) * columns], preferred_element_type=jnp.float32).astype(jnp.bfloat16)
        summed = summed + lax.optimization_barrier(partial_value).astype(jnp.float32)
    return summed

def reference(tokens, mix_gain, query_weight, key_weight, value_weight, gate_weight, out_weight, head_gain, ffn_gain, ffn_gate, ffn_up, ffn_down):
    highest = lax.Precision.HIGHEST
    row_count = tokens.shape[0]
    normed = norm_rows(tokens, mix_gain)

    def project(weight):
        return jnp.dot(normed, weight, preferred_element_type=jnp.float32).astype(jnp.bfloat16)
    positions = jnp.arange(row_count, dtype=jnp.int32) % SEQ
    queries = rotate(project(query_weight).astype(jnp.float32).reshape(row_count, HEADS, DK), positions)
    key_rows = rotate(project(key_weight).astype(jnp.float32).reshape(row_count, HEADS, DK), positions) * DK ** (-0.5)
    value_rows = project(value_weight).astype(jnp.float32).reshape(row_count, HEADS, DV)
    gate_rows = project(gate_weight).astype(jnp.float32)
    decay_rates = log_decay(jnp.arange(HEADS, dtype=jnp.int32), HEADS)
    offsets = jnp.arange(SEQ, dtype=jnp.int32)
    distance = (offsets[:, None] - offsets[None, :]).astype(jnp.float32)
    decay_mask = jnp.where(distance[None] >= 0.0, jnp.exp(jnp.maximum(distance, 0.0)[None] * decay_rates[:, None, None]), 0.0)
    seq_count = row_count // SEQ

    def one_sequence(inputs):
        query_seq, key_seq, value_seq = inputs
        scores = jnp.einsum('ihd,jhd->hij', query_seq, key_seq, precision=highest) * decay_mask
        return jnp.einsum('hij,jhv->ihv', scores, value_seq, precision=highest)
    retained = lax.map(one_sequence, (queries.reshape(seq_count, SEQ, HEADS, DK), key_rows.reshape(seq_count, SEQ, HEADS, DK), value_rows.reshape(seq_count, SEQ, HEADS, DV)))
    retained = retained.reshape(row_count, HEADS, DV)
    center = lax.optimization_barrier(jnp.mean(retained, axis=-1, keepdims=True))
    spread = lax.optimization_barrier(jnp.mean(jnp.square(retained - center), axis=-1, keepdims=True))
    grouped = (retained - center) * lax.rsqrt(spread + epsilon) * head_gain[None]
    mixed = (grouped.reshape(row_count, HEADS * DV) * jax.nn.silu(gate_rows)).astype(jnp.bfloat16)
    residual = (tokens.astype(jnp.float32) + split_sum(mixed, out_weight)).astype(jnp.bfloat16)
    normed_ffn = norm_rows(residual, ffn_gain)
    gate_hidden = jnp.dot(normed_ffn, ffn_gate, preferred_element_type=jnp.float32)
    up_hidden = jnp.dot(normed_ffn, ffn_up, preferred_element_type=jnp.float32)
    hidden = (jax.nn.silu(gate_hidden) * up_hidden).astype(jnp.bfloat16)
    return (residual.astype(jnp.float32) + split_sum(hidden, ffn_down)).astype(jnp.bfloat16)
```

```python
import functools

import jax
import jax.numpy as jnp
from jax import lax
from jax.experimental import pallas as pl
from jax.experimental.pallas import tpu as pltpu
from jax.sharding import PartitionSpec as P

HEADS = 8
DK = 64
DV = 128
BLOCK = 64
SEQ = 256


epsilon = 1e-06
rope_base = 10000.0


def norm_rows(values, gain_row):
    floats = values.astype(jnp.float32)
    scaled = floats * lax.rsqrt(jnp.mean(floats * floats, axis=-1, keepdims=True) + epsilon)
    return (scaled * gain_row).astype(jnp.bfloat16)


def rotate(values, positions):
    half_dim = values.shape[-1] // 2
    frequency = rope_base ** (-jnp.linspace(0.0, 1.0, half_dim, dtype=jnp.float32))
    angles = positions.astype(jnp.float32)[:, None] * frequency[None, :]
    cosine = jnp.cos(angles)[:, None, :]
    sine_part = jnp.sin(angles)[:, None, :]
    paired = values.reshape(values.shape[:-1] + (half_dim, 2))
    leading = paired[..., 0]
    trailing = paired[..., 1]
    turned = jnp.stack(
        [leading * cosine - trailing * sine_part, leading * sine_part + trailing * cosine], axis=-1
    )
    return turned.reshape(values.shape)


def log_decay(head_index, total_heads):
    return jnp.log1p(-jnp.exp2(-5.0 - 4.0 * head_index.astype(jnp.float32) / (total_heads - 1)))


def retention(queries, key_rows, value_rows, decay_rates):
    highest = lax.Precision.HIGHEST
    row_count, head_count = (queries.shape[0], queries.shape[1])
    seq_count = row_count // SEQ
    block_count = SEQ // BLOCK

    def to_blocks(values):
        shaped = values.reshape((seq_count, block_count, BLOCK) + values.shape[1:])
        return jnp.moveaxis(shaped, 1, 0)

    inside = jnp.arange(BLOCK, dtype=jnp.int32)
    gap = (inside[:, None] - inside[None, :]).astype(jnp.float32)
    within_mask = jnp.where(
        gap[None] >= 0.0, jnp.exp(jnp.maximum(gap, 0.0)[None] * decay_rates[:, None, None]), 0.0
    )
    query_scale = jnp.exp((inside + 1).astype(jnp.float32)[:, None] * decay_rates[None, :])
    key_scale = jnp.exp((BLOCK - 1 - inside).astype(jnp.float32)[:, None] * decay_rates[None, :])
    block_decay = jnp.exp(BLOCK * decay_rates)

    def advance(state, inputs):
        query_blk, key_blk, value_blk = inputs
        scores = (
            jnp.einsum("sihd,sjhd->shij", query_blk, key_blk, precision=highest) * within_mask[None]
        )
        local_part = jnp.einsum("shij,sjhv->sihv", scores, value_blk, precision=highest)
        carried = jnp.einsum(
            "sihd,shdv->sihv", query_blk * query_scale[None, :, :, None], state, precision=highest
        )
        update = jnp.einsum(
            "sjhd,sjhv->shdv", key_blk * key_scale[None, :, :, None], value_blk, precision=highest
        )
        return (block_decay[None, :, None, None] * state + update, local_part + carried)

    state_zero = jnp.zeros((seq_count, head_count, DK, DV), jnp.float32)
    _, outputs = lax.scan(
        advance, state_zero, (to_blocks(queries), to_blocks(key_rows), to_blocks(value_rows))
    )
    return jnp.moveaxis(outputs, 0, 1).reshape(row_count, head_count, DV)


def per_device_plain(
    tokens,
    mix_gain,
    query_weight,
    key_weight,
    value_weight,
    gate_weight,
    out_weight,
    head_gain,
    ffn_gain,
    ffn_gate,
    ffn_up,
    ffn_down,
):
    whole_rows = lax.all_gather(tokens, "tp", axis=1, tiled=True)
    row_count = whole_rows.shape[0]
    normed = norm_rows(whole_rows, mix_gain)
    pieces = (
        lax.all_gather(query_weight, "fs", axis=0, tiled=True),
        lax.all_gather(key_weight, "fs", axis=0, tiled=True),
        lax.all_gather(value_weight, "fs", axis=0, tiled=True),
        lax.all_gather(gate_weight, "fs", axis=0, tiled=True),
    )
    query_acc, key_acc, value_acc, gate_acc = tuple(
        (
            jnp.dot(normed, weight_piece, preferred_element_type=jnp.float32)
            for weight_piece in pieces
        )
    )
    heads_here = query_weight.shape[1] // DK
    positions = jnp.arange(row_count, dtype=jnp.int32) % SEQ
    queries = rotate(
        query_acc.astype(jnp.bfloat16).astype(jnp.float32).reshape(row_count, heads_here, DK),
        positions,
    )
    key_rows = rotate(
        key_acc.astype(jnp.bfloat16).astype(jnp.float32).reshape(row_count, heads_here, DK),
        positions,
    ) * DK ** (-0.5)
    value_rows = (
        value_acc.astype(jnp.bfloat16).astype(jnp.float32).reshape(row_count, heads_here, DV)
    )
    gate_rows = gate_acc.astype(jnp.bfloat16).astype(jnp.float32)
    first_head = lax.axis_index("tp") * heads_here
    decay_rates = log_decay(first_head + jnp.arange(heads_here, dtype=jnp.int32), HEADS)
    retained = retention(queries, key_rows, value_rows, decay_rates)
    center = jnp.mean(retained, axis=-1, keepdims=True)
    spread = jnp.mean(jnp.square(retained - center), axis=-1, keepdims=True)
    grouped = (retained - center) * lax.rsqrt(spread + epsilon) * head_gain[None]
    mixed = (grouped.reshape(row_count, heads_here * DV) * jax.nn.silu(gate_rows)).astype(
        jnp.bfloat16
    )
    mixer_terms = jnp.dot(
        mixed,
        lax.all_gather(out_weight, "fs", axis=1, tiled=True),
        preferred_element_type=jnp.float32,
    )
    mixer_share = lax.psum_scatter(
        mixer_terms.astype(jnp.bfloat16), "tp", scatter_dimension=1, tiled=True
    ).astype(jnp.float32)
    resid_shard = (tokens.astype(jnp.float32) + mixer_share).astype(jnp.bfloat16)
    resid_whole = lax.all_gather(resid_shard, "tp", axis=1, tiled=True)
    normed_ffn = norm_rows(resid_whole, ffn_gain)

    def add_rows(weight_piece):
        return jnp.dot(normed_ffn, weight_piece, preferred_element_type=jnp.float32)

    gate_hidden = add_rows(lax.all_gather(ffn_gate, "fs", axis=0, tiled=True))
    up_hidden = add_rows(lax.all_gather(ffn_up, "fs", axis=0, tiled=True))
    hidden = (jax.nn.silu(gate_hidden) * up_hidden).astype(jnp.bfloat16)
    ffn_terms = jnp.dot(
        hidden,
        lax.all_gather(ffn_down, "fs", axis=1, tiled=True),
        preferred_element_type=jnp.float32,
    )
    ffn_share = lax.psum_scatter(
        ffn_terms.astype(jnp.bfloat16), "tp", scatter_dimension=1, tiled=True
    ).astype(jnp.float32)
    return (resid_shard.astype(jnp.float32) + ffn_share).astype(jnp.bfloat16)


def swap_rep(values, ranks):
    count = lax.axis_size("fs")
    pairs = [(r * count + f, (1 - r) * count + f) for r in range(2) for f in ranks]
    return lax.ppermute(values, ("rep", "fs"), pairs)


def gather_half(half):
    far = lax.ppermute(half, "fs", [(0, 2), (1, 3), (2, 0), (3, 1)])
    up = lax.ppermute(half, "fs", [(0, 1), (1, 2), (2, 3)])
    down = lax.ppermute(half, "fs", [(1, 0), (2, 1), (3, 2)])
    relay = lax.ppermute(far, "fs", [(2, 3), (1, 0)])
    far_x = swap_rep(far, (0, 1, 2, 3))
    up_x = swap_rep(up, (1, 2, 3))
    down_x = swap_rep(down, (0, 1, 2))
    relay_x = swap_rep(relay, (0, 3))
    here = lax.axis_index("fs")
    first, last = here == 0, here == 3
    return (
        (2, far, far_x),
        (3, jnp.where(first, relay, up), jnp.where(first, relay_x, up_x)),
        (1, jnp.where(last, relay, down), jnp.where(last, relay_x, down_x)),
    )


def gather_weight(weight, axis):
    rows, columns = weight.shape
    half_rows = rows // 2
    rep, here = lax.axis_index("rep"), lax.axis_index("fs")
    half = lax.dynamic_slice_in_dim(weight, rep * half_rows, half_rows, 0)
    size = [rows, columns]
    size[axis] *= 4
    whole = jnp.zeros(size, weight.dtype)

    def put(whole, piece, rank, row):
        start = (rank * rows + row, 0) if axis == 0 else (row, rank * columns)
        return lax.dynamic_update_slice(whole, piece, start)

    whole = put(whole, weight, here, 0)
    for shift, mine, theirs in gather_half(half):
        rank = (here + shift) % 4
        whole = put(whole, mine, rank, rep * half_rows)
        whole = put(whole, theirs, rank, (1 - rep) * half_rows)
    return whole


def xor_send(values, mask):
    return lax.ppermute(values, "tp", [(i, i ^ mask) for i in range(4)])


def gather_normed(shard, gain):
    across = xor_send(shard, 2)
    beside = xor_send(shard, 1)
    parts = (shard, beside, across, xor_send(across, 1))
    width = shard.shape[1]
    here = lax.axis_index("tp")
    floats = [part.astype(jnp.float32) for part in parts]
    total = sum(jnp.sum(part * part, axis=-1, keepdims=True) for part in floats)
    scale = lax.rsqrt(total / (4 * width) + epsilon)
    whole = jnp.zeros((shard.shape[0], 4 * width), jnp.bfloat16)
    for mask, part in enumerate(floats):
        start = (here ^ mask) * width
        gain_part = lax.dynamic_slice_in_dim(gain, start, width)
        whole = lax.dynamic_update_slice(
            whole, (part * scale * gain_part).astype(jnp.bfloat16), (0, start)
        )
    return whole


def scatter_sum(terms):
    width = terms.shape[1] // 4
    here = lax.axis_index("tp")

    def quarter(mask):
        return lax.dynamic_slice_in_dim(terms, (here ^ mask) * width, width, 1)

    for_across = xor_send(quarter(3), 1)
    beside = xor_send(quarter(1), 1)
    pair = (quarter(2).astype(jnp.float32) + for_across.astype(jnp.float32)).astype(jnp.bfloat16)
    across = xor_send(pair, 2)
    return (
        quarter(0).astype(jnp.float32)
        + beside.astype(jnp.float32)
        + across.astype(jnp.float32)
    )


def mixer_kernel(heads, x_ref, cos_ref, sin_ref, mask_ref, gain_ref, out_ref):
    highest = lax.Precision.HIGHEST
    key_width = heads * DK
    lane = lax.broadcasted_iota(jnp.int32, (SEQ, key_width), 1)
    cosine, sine = cos_ref[...], sin_ref[...]

    def turn(values):
        following = pltpu.roll(values, key_width - 1, 1)
        preceding = pltpu.roll(values, 1, 1)
        other = jnp.where(lane % 2 == 0, -following, preceding)
        return values * cosine + other * sine

    query = turn(x_ref[:, :key_width].astype(jnp.float32))
    key = turn(x_ref[:, key_width : 2 * key_width].astype(jnp.float32)) * DK ** (-0.5)
    for head in range(heads):
        only = jnp.where(lane // DK == head, query, 0.0)
        scores = lax.dot_general(
            only, key, (((1,), (1,)), ((), ())), precision=highest,
            preferred_element_type=jnp.float32,
        ) * mask_ref[head]
        start = 2 * key_width + head * DV
        value = x_ref[:, start : start + DV].astype(jnp.float32)
        retained = jnp.dot(scores, value, precision=highest, preferred_element_type=jnp.float32)
        centered = retained - jnp.mean(retained, axis=-1, keepdims=True)
        spread = jnp.mean(centered * centered, axis=-1, keepdims=True)
        grouped = centered * lax.rsqrt(spread + epsilon) * gain_ref[head : head + 1, :]
        start += heads * DV
        gate = x_ref[:, start : start + DV].astype(jnp.float32)
        out_ref[:, head * DV : (head + 1) * DV] = (grouped * jax.nn.silu(gate)).astype(
            out_ref.dtype
        )


def mix_heads(projected, head_gain):
    heads = head_gain.shape[0]
    rows, width = projected.shape
    first_head = lax.axis_index("tp") * heads
    decay_rates = log_decay(first_head + jnp.arange(heads, dtype=jnp.int32), HEADS)
    offsets = jnp.arange(SEQ, dtype=jnp.int32)
    gap = (offsets[:, None] - offsets[None, :]).astype(jnp.float32)
    mask = jnp.where(
        gap[None] >= 0.0, jnp.exp(jnp.maximum(gap, 0.0)[None] * decay_rates[:, None, None]), 0.0
    )
    frequency = rope_base ** (-jnp.linspace(0.0, 1.0, DK // 2, dtype=jnp.float32))
    angles = offsets.astype(jnp.float32)[:, None] * frequency[None, :]
    cosine = jnp.tile(jnp.repeat(jnp.cos(angles), 2, axis=1), (1, heads))
    sine = jnp.tile(jnp.repeat(jnp.sin(angles), 2, axis=1), (1, heads))
    fixed = lambda shape: pl.BlockSpec(shape, lambda s: (0,) * len(shape))
    return pl.pallas_call(
        functools.partial(mixer_kernel, heads),
        grid=(rows // SEQ,),
        in_specs=[
            pl.BlockSpec((SEQ, width), lambda s: (s, 0)),
            fixed((SEQ, heads * DK)),
            fixed((SEQ, heads * DK)),
            fixed((heads, SEQ, SEQ)),
            fixed((heads, DV)),
        ],
        out_specs=pl.BlockSpec((SEQ, heads * DV), lambda s: (s, 0)),
        out_shape=jax.ShapeDtypeStruct((rows, heads * DV), jnp.bfloat16),
        cost_estimate=pl.CostEstimate(
            flops=12 * rows * SEQ * heads * (DK + DV), bytes_accessed=4 * rows * width, transcendentals=0
        ),
        name="mixer",
    )(projected, cosine, sine, mask, head_gain)


def per_device(
    tokens,
    mix_gain,
    query_weight,
    key_weight,
    value_weight,
    gate_weight,
    out_weight,
    head_gain,
    ffn_gain,
    ffn_gate,
    ffn_up,
    ffn_down,
):
    normed = gather_normed(tokens, mix_gain)
    mix_weight = gather_weight(
        jnp.concatenate((query_weight, key_weight, value_weight, gate_weight), axis=1), 0
    )
    projected = jnp.dot(normed, mix_weight, preferred_element_type=jnp.float32).astype(jnp.bfloat16)
    mixed = mix_heads(projected, head_gain)
    mixer_terms = jnp.dot(
        mixed, gather_weight(out_weight, 1), preferred_element_type=jnp.float32
    ).astype(jnp.bfloat16)
    residual = (tokens.astype(jnp.float32) + scatter_sum(mixer_terms)).astype(jnp.bfloat16)
    normed_ffn = gather_normed(residual, ffn_gain)
    gate_hidden = jnp.dot(normed_ffn, gather_weight(ffn_gate, 0), preferred_element_type=jnp.float32)
    up_hidden = jnp.dot(normed_ffn, gather_weight(ffn_up, 0), preferred_element_type=jnp.float32)
    hidden = (jax.nn.silu(gate_hidden) * up_hidden).astype(jnp.bfloat16)
    ffn_terms = jnp.dot(
        hidden, gather_weight(ffn_down, 1), preferred_element_type=jnp.float32
    ).astype(jnp.bfloat16)
    return (residual.astype(jnp.float32) + scatter_sum(ffn_terms)).astype(jnp.bfloat16)


def solution(mesh):
    shape = mesh.shape
    small = shape["rep"] == 2 and shape["fs"] == 4 and shape["tp"] == 4
    return jax.shard_map(
        per_device if small else per_device_plain,
        mesh=mesh,
        in_specs=(
            P(("rep", "fs"), "tp"),
            P(),
            P("fs", "tp"),
            P("fs", "tp"),
            P("fs", "tp"),
            P("fs", "tp"),
            P("tp", "fs"),
            P("tp", None),
            P(),
            P("fs", "tp"),
            P("fs", "tp"),
            P("tp", "fs"),
        ),
        out_specs=P(("rep", "fs"), "tp"),
        check_vma=False,
    )
```

```python
import functools

import jax
import jax.numpy as jnp
from jax import lax
from jax.experimental import pallas as pl
from jax.experimental.pallas import tpu as pltpu
from jax.sharding import PartitionSpec as P

HEADS = 8
DK = 64
DV = 128
BLOCK = 64
SEQ = 256


epsilon = 1e-06
rope_base = 10000.0


def norm_rows(values, gain_row):
    floats = values.astype(jnp.float32)
    scaled = floats * lax.rsqrt(jnp.mean(floats * floats, axis=-1, keepdims=True) + epsilon)
    return (scaled * gain_row).astype(jnp.bfloat16)


def rotate(values, positions):
    half_dim = values.shape[-1] // 2
    frequency = rope_base ** (-jnp.linspace(0.0, 1.0, half_dim, dtype=jnp.float32))
    angles = positions.astype(jnp.float32)[:, None] * frequency[None, :]
    cosine = jnp.cos(angles)[:, None, :]
    sine_part = jnp.sin(angles)[:, None, :]
    paired = values.reshape(values.shape[:-1] + (half_dim, 2))
    leading = paired[..., 0]
    trailing = paired[..., 1]
    turned = jnp.stack(
        [leading * cosine - trailing * sine_part, leading * sine_part + trailing * cosine], axis=-1
    )
    return turned.reshape(values.shape)


def log_decay(head_index, total_heads):
    return jnp.log1p(-jnp.exp2(-5.0 - 4.0 * head_index.astype(jnp.float32) / (total_heads - 1)))


def retention(queries, key_rows, value_rows, decay_rates):
    highest = lax.Precision.HIGHEST
    row_count, head_count = (queries.shape[0], queries.shape[1])
    seq_count = row_count // SEQ
    block_count = SEQ // BLOCK

    def to_blocks(values):
        shaped = values.reshape((seq_count, block_count, BLOCK) + values.shape[1:])
        return jnp.moveaxis(shaped, 1, 0)

    inside = jnp.arange(BLOCK, dtype=jnp.int32)
    gap = (inside[:, None] - inside[None, :]).astype(jnp.float32)
    within_mask = jnp.where(
        gap[None] >= 0.0, jnp.exp(jnp.maximum(gap, 0.0)[None] * decay_rates[:, None, None]), 0.0
    )
    query_scale = jnp.exp((inside + 1).astype(jnp.float32)[:, None] * decay_rates[None, :])
    key_scale = jnp.exp((BLOCK - 1 - inside).astype(jnp.float32)[:, None] * decay_rates[None, :])
    block_decay = jnp.exp(BLOCK * decay_rates)

    def advance(state, inputs):
        query_blk, key_blk, value_blk = inputs
        scores = (
            jnp.einsum("sihd,sjhd->shij", query_blk, key_blk, precision=highest) * within_mask[None]
        )
        local_part = jnp.einsum("shij,sjhv->sihv", scores, value_blk, precision=highest)
        carried = jnp.einsum(
            "sihd,shdv->sihv", query_blk * query_scale[None, :, :, None], state, precision=highest
        )
        update = jnp.einsum(
            "sjhd,sjhv->shdv", key_blk * key_scale[None, :, :, None], value_blk, precision=highest
        )
        return (block_decay[None, :, None, None] * state + update, local_part + carried)

    state_zero = jnp.zeros((seq_count, head_count, DK, DV), jnp.float32)
    _, outputs = lax.scan(
        advance, state_zero, (to_blocks(queries), to_blocks(key_rows), to_blocks(value_rows))
    )
    return jnp.moveaxis(outputs, 0, 1).reshape(row_count, head_count, DV)


def per_device_plain(
    tokens,
    mix_gain,
    query_weight,
    key_weight,
    value_weight,
    gate_weight,
    out_weight,
    head_gain,
    ffn_gain,
    ffn_gate,
    ffn_up,
    ffn_down,
):
    whole_rows = lax.all_gather(tokens, "tp", axis=1, tiled=True)
    row_count = whole_rows.shape[0]
    normed = norm_rows(whole_rows, mix_gain)
    pieces = (
        lax.all_gather(query_weight, "fs", axis=0, tiled=True),
        lax.all_gather(key_weight, "fs", axis=0, tiled=True),
        lax.all_gather(value_weight, "fs", axis=0, tiled=True),
        lax.all_gather(gate_weight, "fs", axis=0, tiled=True),
    )
    query_acc, key_acc, value_acc, gate_acc = tuple(
        (
            jnp.dot(normed, weight_piece, preferred_element_type=jnp.float32)
            for weight_piece in pieces
        )
    )
    heads_here = query_weight.shape[1] // DK
    positions = jnp.arange(row_count, dtype=jnp.int32) % SEQ
    queries = rotate(
        query_acc.astype(jnp.bfloat16).astype(jnp.float32).reshape(row_count, heads_here, DK),
        positions,
    )
    key_rows = rotate(
        key_acc.astype(jnp.bfloat16).astype(jnp.float32).reshape(row_count, heads_here, DK),
        positions,
    ) * DK ** (-0.5)
    value_rows = (
        value_acc.astype(jnp.bfloat16).astype(jnp.float32).reshape(row_count, heads_here, DV)
    )
    gate_rows = gate_acc.astype(jnp.bfloat16).astype(jnp.float32)
    first_head = lax.axis_index("tp") * heads_here
    decay_rates = log_decay(first_head + jnp.arange(heads_here, dtype=jnp.int32), HEADS)
    retained = retention(queries, key_rows, value_rows, decay_rates)
    center = jnp.mean(retained, axis=-1, keepdims=True)
    spread = jnp.mean(jnp.square(retained - center), axis=-1, keepdims=True)
    grouped = (retained - center) * lax.rsqrt(spread + epsilon) * head_gain[None]
    mixed = (grouped.reshape(row_count, heads_here * DV) * jax.nn.silu(gate_rows)).astype(
        jnp.bfloat16
    )
    mixer_terms = jnp.dot(
        mixed,
        lax.all_gather(out_weight, "fs", axis=1, tiled=True),
        preferred_element_type=jnp.float32,
    )
    mixer_share = lax.psum_scatter(
        mixer_terms.astype(jnp.bfloat16), "tp", scatter_dimension=1, tiled=True
    ).astype(jnp.float32)
    resid_shard = (tokens.astype(jnp.float32) + mixer_share).astype(jnp.bfloat16)
    resid_whole = lax.all_gather(resid_shard, "tp", axis=1, tiled=True)
    normed_ffn = norm_rows(resid_whole, ffn_gain)

    def add_rows(weight_piece):
        return jnp.dot(normed_ffn, weight_piece, preferred_element_type=jnp.float32)

    gate_hidden = add_rows(lax.all_gather(ffn_gate, "fs", axis=0, tiled=True))
    up_hidden = add_rows(lax.all_gather(ffn_up, "fs", axis=0, tiled=True))
    hidden = (jax.nn.silu(gate_hidden) * up_hidden).astype(jnp.bfloat16)
    ffn_terms = jnp.dot(
        hidden,
        lax.all_gather(ffn_down, "fs", axis=1, tiled=True),
        preferred_element_type=jnp.float32,
    )
    ffn_share = lax.psum_scatter(
        ffn_terms.astype(jnp.bfloat16), "tp", scatter_dimension=1, tiled=True
    ).astype(jnp.float32)
    return (resid_shard.astype(jnp.float32) + ffn_share).astype(jnp.bfloat16)


def swap_rep(values, ranks):
    count = lax.axis_size("fs")
    pairs = [(r * count + f, (1 - r) * count + f) for r in range(2) for f in ranks]
    return lax.ppermute(values, ("rep", "fs"), pairs)


def gather_half(half):
    far = lax.ppermute(half, "fs", [(0, 2), (1, 3), (2, 0), (3, 1)])
    up = lax.ppermute(half, "fs", [(0, 1), (1, 2), (2, 3)])
    down = lax.ppermute(half, "fs", [(1, 0), (2, 1), (3, 2)])
    relay = lax.ppermute(far, "fs", [(2, 3), (1, 0)])
    far_x = swap_rep(far, (0, 1, 2, 3))
    up_x = swap_rep(up, (1, 2, 3))
    down_x = swap_rep(down, (0, 1, 2))
    relay_x = swap_rep(relay, (0, 3))
    here = lax.axis_index("fs")
    first, last = here == 0, here == 3
    return (
        (2, far, far_x),
        (3, jnp.where(first, relay, up), jnp.where(first, relay_x, up_x)),
        (1, jnp.where(last, relay, down), jnp.where(last, relay_x, down_x)),
    )


def gather_weight(weight):
    rows, columns = weight.shape
    half_rows = rows // 2
    rep, here = lax.axis_index("rep"), lax.axis_index("fs")
    half = lax.dynamic_slice_in_dim(weight, rep * half_rows, half_rows, 0)
    whole = jnp.zeros((4 * rows, columns), weight.dtype)

    def put(whole, piece, row):
        return lax.dynamic_update_slice(whole, piece, (row, 0))

    whole = put(whole, weight, here * rows)
    for shift, mine, theirs in gather_half(half):
        row = (here + shift) % 4 * rows
        whole = put(whole, mine, row + rep * half_rows)
        whole = put(whole, theirs, row + (1 - rep) * half_rows)
    return whole


def xor_send(values, mask):
    return lax.ppermute(values, "tp", [(i, i ^ mask) for i in range(4)])


def gather_normed(shard, gain):
    across = xor_send(shard, 2)
    beside = xor_send(shard, 1)
    corner = xor_send(across, 1)
    parts = (shard, beside, across, corner)
    width = shard.shape[1]
    here = lax.axis_index("tp")
    floats = [part.astype(jnp.float32) for part in parts]
    total = sum(jnp.sum(part * part, axis=-1, keepdims=True) for part in floats)
    scale = lax.rsqrt(total / (4 * width) + epsilon)
    whole = jnp.zeros((shard.shape[0], 4 * width), jnp.bfloat16)
    for mask, part in enumerate(floats):
        start = (here ^ mask) * width
        gain_part = lax.dynamic_slice_in_dim(gain, start, width)
        whole = lax.dynamic_update_slice(
            whole, (part * scale * gain_part).astype(jnp.bfloat16), (0, start)
        )
    return whole


def product_sum(left, blocks):
    rows = blocks.shape[0] // 4
    here = lax.axis_index("tp")

    def quarter(mask):
        block = lax.dynamic_slice_in_dim(blocks, (here ^ mask) * rows, rows, 0)
        return jnp.dot(left, block, preferred_element_type=jnp.float32)

    corner = quarter(3).astype(jnp.bfloat16)
    corner = xor_send(corner, 1)
    pair = (quarter(2) + corner.astype(jnp.float32)).astype(jnp.bfloat16)
    across = xor_send(pair, 2)
    beside = quarter(1).astype(jnp.bfloat16)
    beside = xor_send(beside, 1)
    own = quarter(0)
    return own + beside.astype(jnp.float32) + across.astype(jnp.float32)


def mixer_kernel(heads, x_ref, cos_ref, sin_ref, mask_ref, gain_ref, out_ref):
    highest = lax.Precision.HIGHEST
    key_width = heads * DK
    lane = lax.broadcasted_iota(jnp.int32, (SEQ, key_width), 1)
    cosine, sine = cos_ref[...], sin_ref[...]

    def turn(values):
        following = pltpu.roll(values, key_width - 1, 1)
        preceding = pltpu.roll(values, 1, 1)
        other = jnp.where(lane % 2 == 0, -following, preceding)
        return values * cosine + other * sine

    query = turn(x_ref[:, :key_width].astype(jnp.float32))
    key = turn(x_ref[:, key_width : 2 * key_width].astype(jnp.float32)) * DK ** (-0.5)
    for head in range(heads):
        only = jnp.where(lane // DK == head, query, 0.0)
        scores = lax.dot_general(
            only, key, (((1,), (1,)), ((), ())), precision=highest,
            preferred_element_type=jnp.float32,
        ) * mask_ref[head]
        start = 2 * key_width + head * DV
        value = x_ref[:, start : start + DV].astype(jnp.float32)
        retained = jnp.dot(scores, value, precision=highest, preferred_element_type=jnp.float32)
        centered = retained - jnp.mean(retained, axis=-1, keepdims=True)
        spread = jnp.mean(centered * centered, axis=-1, keepdims=True)
        grouped = centered * lax.rsqrt(spread + epsilon) * gain_ref[head : head + 1, :]
        start += heads * DV
        gate = x_ref[:, start : start + DV].astype(jnp.float32)
        out_ref[:, head * DV : (head + 1) * DV] = (grouped * jax.nn.silu(gate)).astype(
            out_ref.dtype
        )


def mix_heads(projected, head_gain):
    heads = head_gain.shape[0]
    rows, width = projected.shape
    first_head = lax.axis_index("tp") * heads
    decay_rates = log_decay(first_head + jnp.arange(heads, dtype=jnp.int32), HEADS)
    offsets = jnp.arange(SEQ, dtype=jnp.int32)
    gap = (offsets[:, None] - offsets[None, :]).astype(jnp.float32)
    mask = jnp.where(
        gap[None] >= 0.0, jnp.exp(jnp.maximum(gap, 0.0)[None] * decay_rates[:, None, None]), 0.0
    )
    frequency = rope_base ** (-jnp.linspace(0.0, 1.0, DK // 2, dtype=jnp.float32))
    angles = offsets.astype(jnp.float32)[:, None] * frequency[None, :]
    cosine = jnp.tile(jnp.repeat(jnp.cos(angles), 2, axis=1), (1, heads))
    sine = jnp.tile(jnp.repeat(jnp.sin(angles), 2, axis=1), (1, heads))
    fixed = lambda shape: pl.BlockSpec(shape, lambda s: (0,) * len(shape))
    return pl.pallas_call(
        functools.partial(mixer_kernel, heads),
        grid=(rows // SEQ,),
        in_specs=[
            pl.BlockSpec((SEQ, width), lambda s: (s, 0)),
            fixed((SEQ, heads * DK)),
            fixed((SEQ, heads * DK)),
            fixed((heads, SEQ, SEQ)),
            fixed((heads, DV)),
        ],
        out_specs=pl.BlockSpec((SEQ, heads * DV), lambda s: (s, 0)),
        out_shape=jax.ShapeDtypeStruct((rows, heads * DV), jnp.bfloat16),
        cost_estimate=pl.CostEstimate(
            flops=12 * rows * SEQ * heads * (DK + DV), bytes_accessed=4 * rows * width, transcendentals=0
        ),
        name="mixer",
    )(projected, cosine, sine, mask, head_gain)


def per_device(
    tokens,
    mix_gain,
    query_weight,
    key_weight,
    value_weight,
    gate_weight,
    out_weight,
    head_gain,
    ffn_gain,
    ffn_gate,
    ffn_up,
    ffn_down,
):
    normed = gather_normed(tokens, mix_gain)
    mix_weight = gather_weight(
        jnp.concatenate((query_weight, key_weight, value_weight, gate_weight), axis=1)
    )
    out_blocks = gather_weight(out_weight)
    gate_whole = gather_weight(ffn_gate)
    up_whole = gather_weight(ffn_up)
    down_blocks = gather_weight(ffn_down)
    projected = jnp.dot(normed, mix_weight, preferred_element_type=jnp.float32).astype(jnp.bfloat16)
    mixed = mix_heads(projected, head_gain)
    mixer_share = product_sum(mixed, out_blocks)
    residual = (tokens.astype(jnp.float32) + mixer_share).astype(jnp.bfloat16)
    normed_ffn = gather_normed(residual, ffn_gain)
    gate_hidden = jnp.dot(normed_ffn, gate_whole, preferred_element_type=jnp.float32)
    up_hidden = jnp.dot(normed_ffn, up_whole, preferred_element_type=jnp.float32)
    hidden = (jax.nn.silu(gate_hidden) * up_hidden).astype(jnp.bfloat16)
    ffn_share = product_sum(hidden, down_blocks)
    return (residual.astype(jnp.float32) + ffn_share).astype(jnp.bfloat16)


def layer(*args):
    return per_device(*args)


def solution(mesh):
    shape = mesh.shape
    small = shape["rep"] == 2 and shape["fs"] == 4 and shape["tp"] == 4
    return jax.shard_map(
        layer if small else per_device_plain,
        mesh=mesh,
        in_specs=(
            P(("rep", "fs"), "tp"),
            P(),
            P("fs", "tp"),
            P("fs", "tp"),
            P("fs", "tp"),
            P("fs", "tp"),
            P("tp", "fs"),
            P("tp", None),
            P(),
            P("fs", "tp"),
            P("fs", "tp"),
            P("tp", "fs"),
        ),
        out_specs=P(("rep", "fs"), "tp"),
        check_vma=False,
    )
```
